32 devices in a mesh: sp: 16 (over z, y, x), tp: 2 (over core).
Axes of the slice: x: 2, y: 2, z: 4, core: 2. Of those that a mesh axis runs over, the one named last changes fastest.
Arguments:
- tokens: bfloat16 [4096, 2048], P('sp', 'tp'), may hold values from -6 to 6
- norm_gain: float32 [2048], replicated, may hold values from 0.1 to 1.9
- query_weight: bfloat16 [1024, 2048], P('tp'), may hold values from -0.125 to 0.125
- key_weight: bfloat16 [1024, 2048], P('tp'), may hold values from -0.125 to 0.125
- value_weight: bfloat16 [1024, 2048], P('tp'), may hold values from -0.125 to 0.125
- pool_weight: bfloat16 [1024, 2048], P('tp'), may hold values from -0.125 to 0.125
- query_gain: float32 [64], replicated, may hold values from 0.6 to 6
- key_gain: float32 [64], replicated, may hold values from 0.6 to 6
- cum_gate: float32 [4096, 16], P('sp', 'tp'), as said below
- out_pool_weight: bfloat16 [1024, 2048], P(None, 'tp'), may hold values from -0.1875 to 0.1875
- out_attn_weight: bfloat16 [1024, 2048], P(None, 'tp'), may hold values from -0.1875 to 0.1875
Outputs:
- mixed: bfloat16 [4096, 2048], P('sp', 'tp')
The draws below stay inside these ranges and needn't reach their ends.
Inputs may be any that keep to these rules, and one draw needn't show every extreme that they name: `cum_gate`: in each head the values never rise along the positions.
All inputs are finite; a program needn't handle non-finite values.
Results may differ from the reference program's by a relative error of at most 0.005.
The reference program's roundings to bfloat16 on the way count: a program that leaves them out, or rounds other values in their place, can miss the bound.
Values may be sent and summed in bfloat16 or wider, within the bound.
A program may use at most 128 MiB of HBM per device.

```python
import jax
import jax.numpy as jnp
from jax import lax

D = 2048
ATTENTION_HEADS = 16
HEAD_DIM = 64
POOL_WIDTH = 1024
POOL_GROUPS = 4
TOK_DEV = 256
SEQUENCE_TOKENS = 4096
N_SP = 16


def draw_cum_gate(key, part):
    key_sections = jax.random.split(jax.random.fold_in(key, 7), 5)
    ranking = jax.random.permutation(key_sections[0], ATTENTION_HEADS)
    slow_flag = ranking >= ATTENTION_HEADS // 2
    block_count = SEQUENCE_TOKENS // TOK_DEV
    factor = jnp.exp(jax.random.uniform(key_sections[1], (block_count, 1), jnp.float32, -0.7, 0.7))
    factor = jnp.repeat(factor, TOK_DEV, axis=0)
    roughness = jax.random.uniform(key_sections[2], (SEQUENCE_TOKENS, ATTENTION_HEADS), jnp.float32, 0.5, 1.5)
    base_rate = jnp.where(slow_flag, 0.8 / SEQUENCE_TOKENS, 1.0 / 40.0)
    forget_decay = base_rate[None, :] * factor * roughness
    spike_positions = jax.random.randint(key_sections[3], (2, ATTENTION_HEADS), 0, SEQUENCE_TOKENS)
    spike_length = -jnp.log(jax.random.uniform(key_sections[4], (2, ATTENTION_HEADS), jnp.float32, 0.5, 0.8))
    location_list = jnp.arange(SEQUENCE_TOKENS, dtype=jnp.int32)[None, :, None] == spike_positions[:, None, :]
    spike_events = jnp.sum(jnp.where(location_list, spike_length[:, None, :], 0.0), axis=0)
    spike_events = jnp.where(slow_flag[None, :], spike_events, 0.0)
    return -jnp.cumsum(forget_decay + spike_events, axis=0)


def draw_query_gain(key, part):
    sub_key = jax.random.fold_in(key, 11)
    return jax.random.uniform(sub_key, (HEAD_DIM,), jnp.float32, 0.6, 1.4)


def draw_key_gain(key, part):
    sub_key = jax.random.fold_in(key, 12)
    return jax.random.uniform(sub_key, (HEAD_DIM,), jnp.float32, 0.6, 1.4)


def block_scale(rng, dims, cuts, smallest, largest):
    loudness, own = 1.0, jax.random.fold_in(rng, 6)
    for dim, blocks in cuts:
        draws = jnp.exp(jax.random.uniform(jax.random.fold_in(own, dim), (blocks,), jnp.float32, smallest / len(cuts), largest / len(cuts)))
        loudness = loudness * jnp.repeat(draws, dims[dim] // blocks).reshape([-1 if axis == dim else 1 for axis in range(len(dims))])
    return loudness


def gaussian(stream_key, shape, spread, reach, cuts=(), kind=jnp.bfloat16):
    level = block_scale(stream_key, shape, cuts, -0.22, 0.18) if cuts else 1.0
    values = jax.random.normal(stream_key, shape, jnp.float32) * spread * level
    return jnp.minimum(jnp.maximum(values, -reach), reach).astype(kind)


def setup_inputs(seed: int = 0) -> dict:
    seeds = jax.random.split(jax.random.key(seed), 12)
    tokens = gaussian(seeds[0], (SEQUENCE_TOKENS, D), 1.0, 6.0, ((0, 16), (1, 2)))
    norm_gain = jnp.clip(1.0 + 0.18 * jax.random.normal(seeds[1], (D,), jnp.float32), 0.1, 1.9)
    query_weight = gaussian(seeds[2], (ATTENTION_HEADS * HEAD_DIM, D), D ** -0.5, 0.125, ((0, 2),))
    key_weight = gaussian(seeds[3], (ATTENTION_HEADS * HEAD_DIM, D), D ** -0.5, 0.125, ((0, 2),))
    value_weight = gaussian(seeds[4], (ATTENTION_HEADS * HEAD_DIM, D), D ** -0.5, 0.125, ((0, 2),))
    pool_weight = gaussian(seeds[5], (POOL_WIDTH, D), D ** -0.5, 0.125, ((0, 2),))
    query_gain = draw_query_gain(jax.random.fold_in(seeds[11], 71), 0)
    key_gain = draw_key_gain(jax.random.fold_in(seeds[11], 71), 0)
    cum_gate = draw_cum_gate(jax.random.fold_in(seeds[11], 71), 0)
    out_pool_weight = gaussian(seeds[9], (POOL_WIDTH, D), POOL_WIDTH ** -0.5, 0.1875, ((1, 2),))
    out_attn_weight = gaussian(seeds[10], (ATTENTION_HEADS * HEAD_DIM, D), (ATTENTION_HEADS * HEAD_DIM) ** -0.5, 0.1875, ((1, 2),))
    return dict(tokens=tokens, norm_gain=norm_gain, query_weight=query_weight, key_weight=key_weight, value_weight=value_weight, pool_weight=pool_weight, query_gain=query_gain, key_gain=key_gain, cum_gate=cum_gate, out_pool_weight=out_pool_weight, out_attn_weight=out_attn_weight)


epsilon = 1e-06
masked_fill = -1e+30

def rms_scale(values, gain):
    return values * lax.rsqrt(lax.optimization_barrier(jnp.mean(values * values, axis=-1, keepdims=True)) + epsilon) * gain

def block_partials(query_rows, query_pos, query_gate, key_rows, value_rows, key_pos, key_gate):
    logits = jnp.einsum('qhd,gkhd->qhgk', query_rows.astype(jnp.float32), key_rows.astype(jnp.float32))
    logits = logits + query_gate[:, :, None, None] - jnp.transpose(key_gate, (2, 0, 1))[None]
    allowed = key_pos[None, None, :, :] <= query_pos[:, None, None, None]
    logits = jnp.where(allowed, logits, masked_fill)
    block_max = lax.optimization_barrier(jnp.max(logits, axis=-1))
    weights = jnp.where(allowed, jnp.exp(logits - block_max[..., None]), 0.0)
    totals = lax.optimization_barrier(jnp.sum(weights, axis=-1))
    rounded = lax.optimization_barrier(weights.astype(jnp.bfloat16))
    numerator = jnp.einsum('qhgk,gkhd->qhgd', rounded.astype(jnp.float32), value_rows.astype(jnp.float32))
    return (block_max, totals, numerator)

def pool_reference(values):
    seq_len = values.shape[0]
    group_width = POOL_WIDTH // POOL_GROUPS
    counts = jnp.arange(1, seq_len + 1, dtype=jnp.int32).astype(jnp.float32)[:, None]
    pieces = []
    for group_index in range(POOL_GROUPS):
        window = 2 ** (group_index + 1)
        column = values[:, group_index * group_width:(group_index + 1) * group_width]
        padded = jnp.pad(column, ((window, 0), (0, 0)))
        running = jnp.zeros_like(column)
        for lag_index in range(window):
            running = running + padded[window - lag_index:window - lag_index + seq_len]
        pieces.append(running / jnp.minimum(counts, float(window)))
    return jnp.concatenate(pieces, axis=1) - values

def reference(tokens, norm_gain, query_weight, key_weight, value_weight, pool_weight, query_gain, key_gain, cum_gate, out_pool_weight, out_attn_weight):
    seq_len = tokens.shape[0]
    normed = rms_scale(tokens.astype(jnp.float32), norm_gain).astype(jnp.bfloat16)

    def project(weight):
        return lax.dot_general(normed, weight, (((1,), (1,)), ((), ())), preferred_element_type=jnp.float32)
    query_all = (rms_scale(project(query_weight).reshape(seq_len, ATTENTION_HEADS, HEAD_DIM), query_gain) * HEAD_DIM ** (-0.5)).astype(jnp.bfloat16)
    key_all = rms_scale(project(key_weight).reshape(seq_len, ATTENTION_HEADS, HEAD_DIM), key_gain).astype(jnp.bfloat16)
    value_all = project(value_weight).astype(jnp.bfloat16).reshape(seq_len, ATTENTION_HEADS, HEAD_DIM)
    pool_input = project(pool_weight).astype(jnp.bfloat16)
    pooled = pool_reference(pool_input.astype(jnp.float32)).astype(jnp.bfloat16)
    key_blocks = key_all.reshape(N_SP, TOK_DEV, ATTENTION_HEADS, HEAD_DIM)
    value_blocks = value_all.reshape(N_SP, TOK_DEV, ATTENTION_HEADS, HEAD_DIM)
    gate_blocks = cum_gate.reshape(N_SP, TOK_DEV, ATTENTION_HEADS)
    positions = jnp.arange(seq_len, dtype=jnp.int32)
    key_pos = positions.reshape(N_SP, TOK_DEV)

    def one_block(index):
        start = (index * TOK_DEV).astype(jnp.int32)
        query_rows = lax.dynamic_slice_in_dim(query_all, start, TOK_DEV, 0)
        query_gate = lax.dynamic_slice_in_dim(cum_gate, start, TOK_DEV, 0)
        query_pos = lax.dynamic_slice_in_dim(positions, start, TOK_DEV, 0)
        block_max, totals, numerator = block_partials(query_rows, query_pos, query_gate, key_blocks, value_blocks, key_pos, gate_blocks)
        top = lax.optimization_barrier(jnp.max(block_max, axis=2, keepdims=True))
        scale = jnp.exp(block_max - top)
        denom = lax.optimization_barrier(jnp.sum(scale * totals, axis=2))
        accum = lax.optimization_barrier(jnp.sum(scale[..., None] * numerator, axis=2))
        return accum / denom[..., None]
    attended = lax.map(one_block, jnp.arange(N_SP, dtype=jnp.int32))
    attended = attended.reshape(seq_len, ATTENTION_HEADS * HEAD_DIM).astype(jnp.bfloat16)
    mixed = jnp.dot(pooled, out_pool_weight, preferred_element_type=jnp.float32) + jnp.dot(attended, out_attn_weight, preferred_element_type=jnp.float32)
    return mixed.astype(jnp.bfloat16)
```

```python
import functools

import jax
import jax.numpy as jnp
from jax import lax
from jax.experimental import pallas as pl
from jax.experimental.pallas import tpu as pltpu
from jax.sharding import PartitionSpec as P

HEAD_DIM = 64
POOL_WIDTH = 1024
POOL_GROUPS = 4
PAD = 16
KEY_ROWS = HEAD_DIM + PAD
REACH = 2**POOL_GROUPS

epsilon = 1e-06
masked_fill = -1e30
MESH = pl.DeviceIdType.MESH
NT = (((1,), (1,)), ((), ()))
TN = (((0,), (0,)), ((), ()))
NN = (((1,), (0,)), ((), ()))


def dot(a, b, dims):
    return lax.dot_general(a, b, dims, preferred_element_type=jnp.float32)


def split3(x):
    hi = x.astype(jnp.bfloat16).astype(jnp.float32)
    mid = (x - hi).astype(jnp.bfloat16).astype(jnp.float32)
    low = (x - hi - mid).astype(jnp.bfloat16).astype(jnp.float32)
    return hi, mid, low


def kernel(
    n, T, R, Hh,
    tok, ngain, wq_h, wk_h, wv_h, wp_h, qg, kg, gT, wop_h, woa_h,
    out,
    tokf, nrm, wq, wk, wv, wp, wop, woa, kvs, qs, kvr, qr,
    ext, rim, poolf, att_s, attf, total,
    wsem, tok_ss, tok_rs, kv_ss, kv_rs, q_ss, q_rs, rim_ss, rim_rs,
    pf_ss, pf_rs, at_ss, at_rs, af_ss, af_rs,
):
    me = lax.axis_index("sp")
    t = lax.axis_index("tp")
    L = tok.shape[0]
    F = Hh * HEAD_DIM
    my_head = me // R
    my_r = lax.rem(me, R)
    phase = lax.rem(me, 2 * R)
    out_r = jnp.where(phase < R, phase, 2 * R - 1 - phase)
    out_slot = 2 * (me // (2 * R)) + jnp.where(phase < R, 0, 1)

    def block_of(s):
        return (s // 2) * 2 * R + jnp.where(lax.rem(s, 2) == 0, my_r, 2 * R - 1 - my_r)

    weights = [(wk_h, wk), (wv_h, wv), (wq_h, wq), (wp_h, wp), (wop_h, wop), (woa_h, woa)]
    loads = [pltpu.make_async_copy(a, b, wsem.at[i]) for i, (a, b) in enumerate(weights)]
    for load in loads:
        load.start()

    barrier = pltpu.get_barrier_semaphore()

    @pl.loop(1, n)
    def _(o):
        pl.semaphore_signal(
            barrier, inc=1, device_id=(lax.rem(me + o, n), t), device_id_type=MESH
        )

    for o in range(1, T):
        pl.semaphore_signal(
            barrier, inc=1, device_id=(me, lax.rem(t + o, T)), device_id_type=MESH
        )
    pl.semaphore_wait(barrier, n - 1 + T - 1)

    def sibling(src, dst, ss, rs):
        return [
            pltpu.make_async_remote_copy(
                src_ref=src, dst_ref=dst, send_sem=ss.at[o - 1], recv_sem=rs.at[o - 1],
                device_id=(me, lax.rem(t + o, T)), device_id_type=MESH,
            )
            for o in range(1, T)
        ]

    tok_copies = sibling(tok, tokf.at[t], tok_ss, tok_rs)
    for c in tok_copies:
        c.start()
    tokf[t] = tok[...]
    for c in tok_copies:
        c.wait()

    Dt = tok.shape[1]
    square = jnp.zeros((L, 1), jnp.float32)
    for i in range(T):
        x = tokf[i].astype(jnp.float32)
        square += jnp.sum(x * x, axis=-1, keepdims=True)
    scale = lax.rsqrt(square / (T * Dt) + epsilon)
    for i in range(T):
        cols = slice(i * Dt, (i + 1) * Dt)
        x = tokf[i].astype(jnp.float32)
        nrm[:, cols] = (x * scale * ngain[:, cols]).astype(jnp.bfloat16)

    def head_norm(y, gain):
        y = y.reshape(Hh, HEAD_DIM, L)
        ms = jnp.mean(y * y, axis=1, keepdims=True)
        return y * lax.rsqrt(ms + epsilon) * gain[...][None]

    ghi, gmid, glow = split3(gT[...])
    row = lax.broadcasted_iota(jnp.int32, (PAD, L), 0)

    def gate_rows(h, sign, first):
        pad = jnp.where((row >= 3 - first) & (row < 6 - first), 1.0, 0.0)
        for k, part in enumerate((ghi, gmid, glow)):
            pad = jnp.where(row == k + first, sign * part[h : h + 1], pad)
        return pad.astype(jnp.bfloat16)

    loads[0].wait()
    kvs[:, :HEAD_DIM] = head_norm(dot(wk[...], nrm[...], NT), kg).astype(jnp.bfloat16)
    for h in range(Hh):
        kvs[h, HEAD_DIM:KEY_ROWS] = gate_rows(h, -1.0, 0)
    loads[1].wait()
    kvs[:, KEY_ROWS:] = (
        dot(wv[...], nrm[...], NT).astype(jnp.bfloat16).reshape(Hh, HEAD_DIM, L)
    )

    def kv_copy(o):
        to = lax.rem(me + o, n)
        return pltpu.make_async_remote_copy(
            src_ref=kvs.at[to // R], dst_ref=kvr.at[me],
            send_sem=kv_ss.at[o - 1], recv_sem=kv_rs.at[o - 1],
            device_id=(to, t), device_id_type=MESH,
        )

    def kv_arrival(o):
        return pltpu.make_async_remote_copy(
            src_ref=kvs.at[0], dst_ref=kvr.at[lax.rem(me - o + n, n)],
            send_sem=kv_ss.at[o - 1], recv_sem=kv_rs.at[o - 1],
            device_id=(lax.rem(me + o, n), t), device_id_type=MESH,
        )

    @pl.loop(1, n)
    def _(o):
        kv_copy(o).start()

    kvr[me] = kvs[my_head]

    loads[2].wait()
    q = head_norm(dot(wq[...], nrm[...], NT), qg) * HEAD_DIM ** (-0.5)
    qs[:, :HEAD_DIM] = q.astype(jnp.bfloat16)
    for h in range(Hh):
        qs[h, HEAD_DIM:KEY_ROWS] = gate_rows(h, 1.0, 3)

    def q_copy(h):
        return pltpu.make_async_remote_copy(
            src_ref=qs.at[h], dst_ref=qr.at[out_slot],
            send_sem=q_ss.at[h], recv_sem=q_rs.at[out_slot],
            device_id=(h * R + out_r, t), device_id_type=MESH,
        )

    def q_arrival(s):
        return pltpu.make_async_remote_copy(
            src_ref=qs.at[0], dst_ref=qr.at[s],
            send_sem=q_ss.at[0], recv_sem=q_rs.at[s],
            device_id=(block_of(s), t), device_id_type=MESH,
        )

    @pl.loop(0, Hh)
    def _(h):
        @pl.when(h * R + out_r != me)
        def _():
            q_copy(h).start()

        @pl.when(h * R + out_r == me)
        def _():
            qr[out_slot] = qs[h]

    loads[3].wait()
    pool_input = dot(nrm[...], wp[...], NT).astype(jnp.bfloat16)
    ext[...] = pool_input[L - REACH :]
    rim_copy = pltpu.make_async_remote_copy(
        src_ref=ext, dst_ref=rim, send_sem=rim_ss, recv_sem=rim_rs,
        device_id=(lax.rem(me + 1, n), t), device_id_type=MESH,
    )

    rim_copy.start()
    rim_copy.wait()
    before = jnp.where(me == 0, 0.0, rim[...].astype(jnp.float32))
    current = pool_input.astype(jnp.float32)
    running = jnp.concatenate([before, current], axis=0)
    width_here = current.shape[1]
    channel = t * width_here + lax.broadcasted_iota(jnp.int32, (1, width_here), 1)
    group = channel // (POOL_WIDTH // POOL_GROUPS)
    counts = (me * L + 1 + lax.broadcasted_iota(jnp.int32, (L, 1), 0)).astype(jnp.float32)
    pooled = jnp.zeros_like(current)
    for g in range(POOL_GROUPS):
        lag = 2**g
        running = running + jnp.concatenate(
            [jnp.zeros((lag, width_here), jnp.float32), running[:-lag]], axis=0
        )
        average = running[REACH:] / jnp.minimum(counts, float(2 * lag))
        pooled = jnp.where(group == g, average, pooled)
    poolf[t] = (pooled - current).astype(jnp.bfloat16)
    pool_copies = sibling(poolf.at[t], poolf.at[t], pf_ss, pf_rs)
    for c in pool_copies:
        c.start()

    @pl.loop(1, n)
    def _(o):
        kv_arrival(o).wait_recv()

    def scores(q_block, j):
        return dot(kvr[j, :KEY_ROWS], q_block, TN)

    def absorb(state, s, values):
        top, den, acc = state
        new_top = jnp.maximum(top, jnp.max(s, axis=0, keepdims=True))
        old = jnp.exp(top - new_top)
        w = jnp.exp(s - new_top)
        den = den * old + jnp.sum(w, axis=0, keepdims=True)
        acc = acc * old + dot(values, w.astype(jnp.bfloat16), NN)
        return new_top, den, acc

    allowed = lax.broadcasted_iota(jnp.int32, (L, L), 0) <= lax.broadcasted_iota(
        jnp.int32, (L, L), 1
    )

    def at_copy(s):
        return pltpu.make_async_remote_copy(
            src_ref=att_s.at[s], dst_ref=attf.at[t, my_head],
            send_sem=at_ss.at[s], recv_sem=at_rs.at[my_head],
            device_id=(block_of(s), t), device_id_type=MESH,
        )

    def at_arrival(h):
        return pltpu.make_async_remote_copy(
            src_ref=att_s.at[0], dst_ref=attf.at[t, h],
            send_sem=at_ss.at[0], recv_sem=at_rs.at[h],
            device_id=(h * R + out_r, t), device_id_type=MESH,
        )

    @pl.loop(0, Hh)
    def _(s):
        b = block_of(s)

        @pl.when(b != me)
        def _():
            q_arrival(s).wait_recv()

        q_block = qr[s]
        first = jnp.where(allowed, scores(q_block, b), masked_fill)
        state = (
            jnp.full((1, L), masked_fill, jnp.float32),
            jnp.zeros((1, L), jnp.float32),
            jnp.zeros((HEAD_DIM, L), jnp.float32),
        )
        state = absorb(state, first, kvr[b, KEY_ROWS:])

        def single(j, state):
            return absorb(state, scores(q_block, j), kvr[j, KEY_ROWS:])

        def pair(p, state):
            j = 2 * p
            both = jnp.concatenate([scores(q_block, j), scores(q_block, j + 1)], axis=0)
            values = jnp.concatenate([kvr[j, KEY_ROWS:], kvr[j + 1, KEY_ROWS:]], axis=1)
            return absorb(state, both, values)

        state = lax.fori_loop(0, b // 2, pair, state)
        state = lax.fori_loop(2 * (b // 2), b, single, state)
        att_s[s] = (state[2] / state[1]).astype(jnp.bfloat16)

        @pl.when(b != me)
        def _():
            at_copy(s).start()

        @pl.when(b == me)
        def _():
            attf[t, my_head] = att_s[s]

    for c in pool_copies:
        c.wait()
    loads[4].wait()
    for i in range(T):
        part = dot(poolf[i], wop[i * width_here : (i + 1) * width_here], NN)
        if i == 0:
            total[...] = part
        else:
            total[...] += part

    @pl.loop(0, Hh)
    def _(h):
        @pl.when(h * R + out_r != me)
        def _():
            at_arrival(h).wait_recv()

    att_copies = sibling(attf.at[t], attf.at[t], af_ss, af_rs)
    for c in att_copies:
        c.start()
    loads[5].wait()

    def attn_part(i):
        rows = pl.ds(pl.multiple_of(i * F, F), F)
        return dot(attf[i].reshape(F, L), woa[rows], TN)

    result = total[...] + attn_part(t)
    for o in range(1, T):
        att_copies[o - 1].wait()
        result = result + attn_part(lax.rem(t - o + T, T))
    out[...] = result.astype(jnp.bfloat16)

    @pl.loop(1, n)
    def _(o):
        kv_copy(o).wait_send()

    @pl.loop(0, Hh)
    def _(h):
        @pl.when(h * R + out_r != me)
        def _():
            q_copy(h).wait_send()

        @pl.when(block_of(h) != me)
        def _():
            at_copy(h).wait_send()


def solution(mesh):
    n, T = mesh.shape["sp"], mesh.shape["tp"]

    def per_device(
        tokens, norm_gain, query_weight, key_weight, value_weight, pool_weight,
        query_gain, key_gain, cum_gate, out_pool_weight, out_attn_weight,
    ):
        L, Dt = tokens.shape
        Hh = cum_gate.shape[1]
        R = n // Hh
        F = Hh * HEAD_DIM
        Fp = pool_weight.shape[0]
        bf, f32 = jnp.bfloat16, jnp.float32
        vmem = pl.BlockSpec(memory_space=pltpu.VMEM)
        hbm = pl.BlockSpec(memory_space=pl.ANY)
        dma = pltpu.SemaphoreType.DMA
        S = max(T - 1, 1)
        return pl.pallas_call(
            functools.partial(kernel, n, T, R, Hh),
            out_shape=jax.ShapeDtypeStruct((L, Dt), bf),
            in_specs=[vmem, vmem, hbm, hbm, hbm, hbm, vmem, vmem, vmem, hbm, hbm],
            out_specs=vmem,
            scratch_shapes=[
                pltpu.VMEM((T, L, Dt), bf),
                pltpu.VMEM((L, T * Dt), bf),
                pltpu.VMEM(query_weight.shape, bf),
                pltpu.VMEM(key_weight.shape, bf),
                pltpu.VMEM(value_weight.shape, bf),
                pltpu.VMEM(pool_weight.shape, bf),
                pltpu.VMEM(out_pool_weight.shape, bf),
                pltpu.VMEM(out_attn_weight.shape, bf),
                pltpu.VMEM((Hh, KEY_ROWS + HEAD_DIM, L), bf),
                pltpu.VMEM((Hh, KEY_ROWS, L), bf),
                pltpu.VMEM((n, KEY_ROWS + HEAD_DIM, L), bf),
                pltpu.VMEM((Hh, KEY_ROWS, L), bf),
                pltpu.VMEM((REACH, Fp), bf),
                pltpu.VMEM((REACH, Fp), bf),
                pltpu.VMEM((T, L, Fp), bf),
                pltpu.VMEM((Hh, HEAD_DIM, L), bf),
                pltpu.VMEM((T, Hh, HEAD_DIM, L), bf),
                pltpu.VMEM((L, Dt), f32),
                dma((6,)),
                dma((S,)), dma((S,)),
                dma((n - 1,)), dma((n - 1,)),
                dma((Hh,)), dma((Hh,)),
                dma, dma,
                dma((S,)), dma((S,)),
                dma((Hh,)), dma((Hh,)),
                dma((S,)), dma((S,)),
            ],
            compiler_params=pltpu.CompilerParams(
                collective_id=0, has_side_effects=True, vmem_limit_bytes=56 * 2**20
            ),
        )(
            tokens, norm_gain.reshape(1, -1), query_weight, key_weight, value_weight,
            pool_weight, query_gain.reshape(-1, 1), key_gain.reshape(-1, 1), cum_gate.T,
            out_pool_weight, out_attn_weight,
        )

    return jax.shard_map(
        per_device,
        mesh=mesh,
        in_specs=(
            P("sp", "tp"), P(), P("tp", None), P("tp", None), P("tp", None), P("tp", None),
            P(), P(), P("sp", "tp"), P(None, "tp"), P(None, "tp"),
        ),
        out_specs=P("sp", "tp"),
        check_vma=False,
    )
```

```python
import functools

import jax
import jax.numpy as jnp
from jax import lax
from jax.experimental import pallas as pl
from jax.experimental.pallas import tpu as pltpu
from jax.sharding import PartitionSpec as P

HEAD_DIM = 64
POOL_WIDTH = 1024
POOL_GROUPS = 4
PAD = 16
KEY_ROWS = HEAD_DIM + PAD
REACH = 2**POOL_GROUPS

epsilon = 1e-06
masked_fill = -1e30
MESH = pl.DeviceIdType.MESH
NT = (((1,), (1,)), ((), ()))
TN = (((0,), (0,)), ((), ()))
NN = (((1,), (0,)), ((), ()))


def dot(a, b, dims):
    return lax.dot_general(a, b, dims, preferred_element_type=jnp.float32)


def split3(x):
    hi = x.astype(jnp.bfloat16).astype(jnp.float32)
    mid = (x - hi).astype(jnp.bfloat16).astype(jnp.float32)
    low = (x - hi - mid).astype(jnp.bfloat16).astype(jnp.float32)
    return hi, mid, low


def kernel(
    n, T, R, Hh,
    tok, ngain, wq_h, wk_h, wv_h, wp_h, qg, kg, gT, wop_h, woa_h,
    out,
    tokf, nrm, wq, wk, wv, wp, wop, woa, kvs, qs, kvr, qr,
    ext, rim, poolf, att_s, attf, total, keys, top, den, acc,
    wsem, tok_ss, tok_rs, kv_ss, kv_rs, fw_ss, q_ss, q_rs, rim_ss, rim_rs,
    pf_ss, pf_rs, at_ss, at_rs, af_ss, af_rs,
):
    me = lax.axis_index("sp")
    t = lax.axis_index("tp")
    L = tok.shape[0]
    F = Hh * HEAD_DIM
    C = n // (T * Hh)
    span = n // T
    my_tp = me // (C * Hh)
    my_head = lax.rem(me // C, Hh)
    my_r = lax.rem(me, C) * T + t
    relay = lax.rem(me, T)
    seat = lax.rem(me, span)
    phase = lax.rem(me, 2 * R)
    out_r = jnp.where(phase < R, phase, 2 * R - 1 - phase)
    out_slot = 2 * (me // (2 * R)) + jnp.where(phase < R, 0, 1)

    def block_of(s):
        return (s // 2) * 2 * R + jnp.where(lax.rem(s, 2) == 0, my_r, 2 * R - 1 - my_r)

    weights = [(wq_h, wq), (wk_h, wk), (wv_h, wv), (wp_h, wp), (wop_h, wop), (woa_h, woa)]
    loads = [pltpu.make_async_copy(a, b, wsem.at[i]) for i, (a, b) in enumerate(weights)]
    for load in loads:
        load.start()

    barrier = pltpu.get_barrier_semaphore()

    @pl.loop(1, n * T)
    def _(o):
        other = lax.rem(me * T + t + o, n * T)
        pl.semaphore_signal(
            barrier, inc=1, device_id=(other // T, lax.rem(other, T)), device_id_type=MESH
        )

    pl.semaphore_wait(barrier, n * T - 1)

    def sibling(src, dst, ss, rs):
        return [
            pltpu.make_async_remote_copy(
                src_ref=src, dst_ref=dst, send_sem=ss.at[o - 1], recv_sem=rs.at[o - 1],
                device_id=(me, lax.rem(t + o, T)), device_id_type=MESH,
            )
            for o in range(1, T)
        ]

    tok_copies = sibling(tok, tokf.at[t], tok_ss, tok_rs)
    for c in tok_copies:
        c.start()
    tokf[t] = tok[...]
    for c in tok_copies:
        c.wait()

    Dt = tok.shape[1]
    square = jnp.zeros((L, 1), jnp.float32)
    for i in range(T):
        x = tokf[i].astype(jnp.float32)
        square += jnp.sum(x * x, axis=-1, keepdims=True)
    scale = lax.rsqrt(square / (T * Dt) + epsilon)
    for i in range(T):
        cols = slice(i * Dt, (i + 1) * Dt)
        x = tokf[i].astype(jnp.float32)
        nrm[:, cols] = (x * scale * ngain[:, cols]).astype(jnp.bfloat16)

    def head_norm(y, gain):
        y = y.reshape(Hh, HEAD_DIM, L)
        ms = jnp.mean(y * y, axis=1, keepdims=True)
        square_ids = [
            lax.broadcasted_iota(jnp.int32, (HEAD_DIM, HEAD_DIM), d) for d in (0, 1)
        ]
        column = jnp.sum(
            jnp.where(square_ids[0] == square_ids[1], gain[...], 0.0), axis=1, keepdims=True
        )
        return y * lax.rsqrt(ms + epsilon) * column[None]

    ghi, gmid, glow = split3(gT[...])
    row = lax.broadcasted_iota(jnp.int32, (PAD, L), 0)

    def gate_rows(h, sign, first):
        pad = jnp.where((row >= 3 - first) & (row < 6 - first), 1.0, 0.0)
        for k, part in enumerate((ghi, gmid, glow)):
            pad = jnp.where(row == k + first, sign * part[h : h + 1], pad)
        return pad.astype(jnp.bfloat16)

    loads[0].wait()
    q = head_norm(dot(wq[...], nrm[...], NT), qg) * HEAD_DIM ** (-0.5)
    qs[:, :HEAD_DIM] = q.astype(jnp.bfloat16)
    for h in range(Hh):
        qs[h, HEAD_DIM:KEY_ROWS] = gate_rows(h, 1.0, 3)

    def is_me(device):
        return (device[0] == me) & (device[1] == t)

    def q_home(h):
        return ((t * Hh + h) * C + out_r // T, lax.rem(out_r, T))

    def q_source(s):
        return (block_of(s), my_tp)

    def q_copy(h):
        return pltpu.make_async_remote_copy(
            src_ref=qs.at[h], dst_ref=qr.at[out_slot],
            send_sem=q_ss.at[h], recv_sem=q_rs.at[out_slot],
            device_id=q_home(h), device_id_type=MESH,
        )

    def q_arrival(s):
        return pltpu.make_async_remote_copy(
            src_ref=qs.at[0], dst_ref=qr.at[s],
            send_sem=q_ss.at[0], recv_sem=q_rs.at[s],
            device_id=q_source(s), device_id_type=MESH,
        )

    @pl.loop(0, Hh)
    def _(o):
        h = lax.rem(me + o, Hh)

        @pl.when(jnp.logical_not(is_me(q_home(h))))
        def _():
            q_copy(h).start()

        @pl.when(is_me(q_home(h)))
        def _():
            qr[out_slot] = qs[h]

    loads[1].wait()
    kvs[:, :HEAD_DIM] = head_norm(dot(wk[...], nrm[...], NT), kg).astype(jnp.bfloat16)
    for h in range(Hh):
        kvs[h, HEAD_DIM:KEY_ROWS] = gate_rows(h, -1.0, 0)
    loads[2].wait()
    kvs[:, KEY_ROWS:] = (
        dot(wv[...], nrm[...], NT).astype(jnp.bfloat16).reshape(Hh, HEAD_DIM, L)
    )

    def kv_home(k):
        return (t * span + k, relay)

    def kv_copy(k):
        return pltpu.make_async_remote_copy(
            src_ref=kvs.at[k // C], dst_ref=kvr.at[me],
            send_sem=kv_ss.at[k], recv_sem=kv_rs.at[me],
            device_id=kv_home(k), device_id_type=MESH,
        )

    def kv_arrival(j, tp):
        return pltpu.make_async_remote_copy(
            src_ref=kvs.at[0], dst_ref=kvr.at[j],
            send_sem=kv_ss.at[0], recv_sem=kv_rs.at[j],
            device_id=(me, tp), device_id_type=MESH,
        )

    def kv_forward(j, o):
        return pltpu.make_async_remote_copy(
            src_ref=kvr.at[j], dst_ref=kvr.at[j],
            send_sem=fw_ss.at[o - 1, j], recv_sem=kv_rs.at[j],
            device_id=(me, lax.rem(t + o, T)), device_id_type=MESH,
        )

    @pl.loop(0, span)
    def _(o):
        k = lax.rem(me + o, span)

        @pl.when(jnp.logical_not(is_me(kv_home(k))))
        def _():
            kv_copy(k).start()

        @pl.when(is_me(kv_home(k)))
        def _():
            kvr[me] = kvs[k // C]

    loads[3].wait()
    pool_input = dot(nrm[...], wp[...], NT).astype(jnp.bfloat16)
    ext[...] = pool_input[L - REACH :]
    rim_copy = pltpu.make_async_remote_copy(
        src_ref=ext, dst_ref=rim, send_sem=rim_ss, recv_sem=rim_rs,
        device_id=(lax.rem(me + 1, n), t), device_id_type=MESH,
    )

    rim_copy.start()
    rim_copy.wait()
    before = jnp.where(me == 0, 0.0, rim[...].astype(jnp.float32))
    current = pool_input.astype(jnp.float32)
    running = jnp.concatenate([before, current], axis=0)
    width_here = current.shape[1]
    channel = t * width_here + lax.broadcasted_iota(jnp.int32, (1, width_here), 1)
    group = channel // (POOL_WIDTH // POOL_GROUPS)
    counts = (me * L + 1 + lax.broadcasted_iota(jnp.int32, (L, 1), 0)).astype(jnp.float32)
    pooled = jnp.zeros_like(current)
    for g in range(POOL_GROUPS):
        lag = 2**g
        running = running + jnp.concatenate(
            [jnp.zeros((lag, width_here), jnp.float32), running[:-lag]], axis=0
        )
        average = running[REACH:] / jnp.minimum(counts, float(2 * lag))
        pooled = jnp.where(group == g, average, pooled)
    poolf[t] = (pooled - current).astype(jnp.bfloat16)
    pool_copies = sibling(poolf.at[t], poolf.at[t], pf_ss, pf_rs)
    for c in pool_copies:
        c.start()

    for c in pool_copies:
        c.wait()
    loads[4].wait()
    for i in range(T):
        part = dot(poolf[i], wop[i * width_here : (i + 1) * width_here], NN)
        if i == 0:
            total[...] = part
        else:
            total[...] += part

    top[...] = jnp.full(top.shape, masked_fill, jnp.float32)
    den[...] = jnp.zeros(den.shape, jnp.float32)
    acc[...] = jnp.zeros(acc.shape, jnp.float32)
    allowed = lax.broadcasted_iota(jnp.int32, (L, L), 0) <= lax.broadcasted_iota(
        jnp.int32, (L, L), 1
    )

    @pl.loop(0, Hh)
    def _(s):
        @pl.when(jnp.logical_not(is_me(q_source(s))))
        def _():
            q_arrival(s).wait_recv()

    def absorb(slots, j, masked):
        logits = [dot(keys[...], qr[s], NN) for s in slots]
        if masked:
            logits = [jnp.where(allowed, x, masked_fill) for x in logits]
        new = [jnp.maximum(top[s], jnp.max(x, axis=0, keepdims=True)) for s, x in zip(slots, logits)]
        w = [jnp.exp(x - m) for x, m in zip(logits, new)]
        parts = [dot(kvr[j, KEY_ROWS:], x.astype(jnp.bfloat16), NN) for x in w]
        for s, m, x, part in zip(slots, new, w, parts):
            old = jnp.exp(top[s] - m)
            top[s] = m
            den[s] = den[s] * old + jnp.sum(x, axis=0, keepdims=True)
            acc[s] = acc[s] * old + part

    def attend(j):
        keys[...] = jnp.transpose(kvr[j, :KEY_ROWS])
        p = lax.rem(j, 2 * R)
        low = 2 * (j // (2 * R)) + jnp.where(p > my_r, 1, 0) + jnp.where(p > 2 * R - 1 - my_r, 1, 0)
        diagonal = (p == my_r) | (p == 2 * R - 1 - my_r)

        @pl.when(diagonal)
        def _():
            absorb([low], j, True)

        low = low + jnp.where(diagonal, 1, 0)
        pairs = (Hh - low) // 2

        @pl.loop(0, pairs)
        def _(i):
            absorb([low + 2 * i, low + 2 * i + 1], j, False)

        @pl.when(lax.rem(Hh - low, 2) == 1)
        def _():
            absorb([Hh - 1], j, False)

    @pl.loop(0, span // T)
    def _(step):
        for u in range(T):
            k = step * T + lax.rem(seat - t - u + 2 * T, T)
            base = lax.rem(seat - k + span, span)
            for m in range(T):
                j = base + m * span

                @pl.when(jnp.logical_not((u == 0) & is_me((j, my_tp))))
                def _():
                    kv_arrival(j, lax.rem(t + 1, T)).wait_recv()

                if u == 0:
                    for o in range(1, T):
                        kv_forward(j, o).start()

            @pl.loop(0, T)
            def _(m):
                attend(base + m * span)

    def at_copy(s):
        return pltpu.make_async_remote_copy(
            src_ref=att_s.at[s], dst_ref=attf.at[my_tp, my_head],
            send_sem=at_ss.at[s], recv_sem=at_rs.at[my_head],
            device_id=q_source(s), device_id_type=MESH,
        )

    def at_arrival(h):
        return pltpu.make_async_remote_copy(
            src_ref=att_s.at[0], dst_ref=attf.at[t, h],
            send_sem=at_ss.at[0], recv_sem=at_rs.at[h],
            device_id=q_home(h), device_id_type=MESH,
        )

    @pl.loop(0, Hh)
    def _(s):
        att_s[s] = (acc[s] / den[s]).astype(jnp.bfloat16)

        @pl.when(jnp.logical_not(is_me(q_source(s))))
        def _():
            at_copy(s).start()

        @pl.when(is_me(q_source(s)))
        def _():
            attf[t, my_head] = att_s[s]

    @pl.loop(0, Hh)
    def _(h):
        @pl.when(jnp.logical_not(is_me(q_home(h))))
        def _():
            at_arrival(h).wait_recv()

    att_copies = sibling(attf.at[t], attf.at[t], af_ss, af_rs)
    for c in att_copies:
        c.start()
    loads[5].wait()

    def attn_part(i):
        rows = pl.ds(pl.multiple_of(i * F, F), F)
        return dot(attf[i].reshape(F, L), woa[rows], TN)

    result = total[...] + attn_part(t)
    for o in range(1, T):
        att_copies[o - 1].wait()
        result = result + attn_part(lax.rem(t - o + T, T))
    out[...] = result.astype(jnp.bfloat16)

    @pl.loop(0, span)
    def _(k):
        @pl.when(jnp.logical_not(is_me(kv_home(k))))
        def _():
            kv_copy(k).wait_send()

        for o in range(1, T):
            kv_forward(k * T + t, o).wait_send()

    @pl.loop(0, Hh)
    def _(h):
        @pl.when(jnp.logical_not(is_me(q_home(h))))
        def _():
            q_copy(h).wait_send()

        @pl.when(jnp.logical_not(is_me(q_source(h))))
        def _():
            at_copy(h).wait_send()


def solution(mesh):
    n, T = mesh.shape["sp"], mesh.shape["tp"]

    def per_device(
        tokens, norm_gain, query_weight, key_weight, value_weight, pool_weight,
        query_gain, key_gain, cum_gate, out_pool_weight, out_attn_weight,
    ):
        L, Dt = tokens.shape
        Hh = cum_gate.shape[1]
        R = n // Hh
        F = Hh * HEAD_DIM
        Fp = pool_weight.shape[0]
        bf, f32 = jnp.bfloat16, jnp.float32
        vmem = pl.BlockSpec(memory_space=pltpu.VMEM)
        hbm = pl.BlockSpec(memory_space=pl.ANY)
        dma = pltpu.SemaphoreType.DMA
        S = max(T - 1, 1)
        return pl.pallas_call(
            functools.partial(kernel, n, T, R, Hh),
            out_shape=jax.ShapeDtypeStruct((L, Dt), bf),
            in_specs=[vmem, vmem, hbm, hbm, hbm, hbm, vmem, vmem, vmem, hbm, hbm],
            out_specs=vmem,
            scratch_shapes=[
                pltpu.VMEM((T, L, Dt), bf),
                pltpu.VMEM((L, T * Dt), bf),
                pltpu.VMEM(query_weight.shape, bf),
                pltpu.VMEM(key_weight.shape, bf),
                pltpu.VMEM(value_weight.shape, bf),
                pltpu.VMEM(pool_weight.shape, bf),
                pltpu.VMEM(out_pool_weight.shape, bf),
                pltpu.VMEM(out_attn_weight.shape, bf),
                pltpu.VMEM((Hh, KEY_ROWS + HEAD_DIM, L), bf),
                pltpu.VMEM((Hh, KEY_ROWS, L), bf),
                pltpu.VMEM((n, KEY_ROWS + HEAD_DIM, L), bf),
                pltpu.VMEM((Hh, KEY_ROWS, L), bf),
                pltpu.VMEM((REACH, Fp), bf),
                pltpu.VMEM((REACH, Fp), bf),
                pltpu.VMEM((T, L, Fp), bf),
                pltpu.VMEM((Hh, HEAD_DIM, L), bf),
                pltpu.VMEM((T, Hh, HEAD_DIM, L), bf),
                pltpu.VMEM((L, Dt), f32),
                pltpu.VMEM((L, KEY_ROWS), bf),
                pltpu.VMEM((Hh, 1, L), f32),
                pltpu.VMEM((Hh, 1, L), f32),
                pltpu.VMEM((Hh, HEAD_DIM, L), f32),
                dma((6,)),
                dma((S,)), dma((S,)),
                dma((n // T,)), dma((n,)), dma((S, n)),
                dma((Hh,)), dma((Hh,)),
                dma, dma,
                dma((S,)), dma((S,)),
                dma((Hh,)), dma((Hh,)),
                dma((S,)), dma((S,)),
            ],
            compiler_params=pltpu.CompilerParams(
                collective_id=0, has_side_effects=True, vmem_limit_bytes=56 * 2**20
            ),
        )(
            tokens, norm_gain.reshape(1, -1), query_weight, key_weight, value_weight,
            pool_weight, query_gain.reshape(1, -1), key_gain.reshape(1, -1), cum_gate.T,
            out_pool_weight, out_attn_weight,
        )

    return jax.shard_map(
        per_device,
        mesh=mesh,
        in_specs=(
            P("sp", "tp"), P(), P("tp", None), P("tp", None), P("tp", None), P("tp", None),
            P(), P(), P("sp", "tp"), P(None, "tp"), P(None, "tp"),
        ),
        out_specs=P("sp", "tp"),
        check_vma=False,
    )
```

```python
import functools

import jax
import jax.numpy as jnp
from jax import lax
from jax.experimental import pallas as pl
from jax.experimental.pallas import tpu as pltpu
from jax.sharding import PartitionSpec as P

HEAD_DIM = 64
POOL_WIDTH = 1024
POOL_GROUPS = 4
PAD = 16
KEY_ROWS = HEAD_DIM + PAD
REACH = 2**POOL_GROUPS

epsilon = 1e-06
masked_fill = -1e30
MESH = pl.DeviceIdType.MESH
NT = (((1,), (1,)), ((), ()))
TN = (((0,), (0,)), ((), ()))
NN = (((1,), (0,)), ((), ()))


def dot(a, b, dims):
    return lax.dot_general(a, b, dims, preferred_element_type=jnp.float32)


def split3(x):
    hi = x.astype(jnp.bfloat16).astype(jnp.float32)
    mid = (x - hi).astype(jnp.bfloat16).astype(jnp.float32)
    low = (x - hi - mid).astype(jnp.bfloat16).astype(jnp.float32)
    return hi, mid, low


def kernel(
    n, T, R, Hh,
    tok, ngain, wq_h, wk_h, wv_h, wp_h, qg, kg, gT, wop_h, woa_h,
    out,
    tokf, nrm, wq, wk, wv, wp, wop, woa, kvs, qs, kvr, qr,
    ext, rim, poolf, att_s, attf, total, keys, top, den, acc,
    wsem, tok_ss, tok_rs, kv_ss, kv_rs, fw_ss, q_ss, q_rs, rim_ss, rim_rs,
    pf_ss, pf_rs, at_ss, at_rs, af_ss, af_rs,
):
    me = lax.axis_index("sp")
    t = lax.axis_index("tp")
    L = tok.shape[0]
    F = Hh * HEAD_DIM
    C = n // (T * Hh)
    span = n // T
    my_tp = me // (C * Hh)
    my_head = lax.rem(me // C, Hh)
    my_r = lax.rem(me, C) * T + t
    relay = lax.rem(me, T)
    seat = lax.rem(me, span)
    phase = lax.rem(me, 2 * R)
    out_r = jnp.where(phase < R, phase, 2 * R - 1 - phase)
    out_slot = 2 * (me // (2 * R)) + jnp.where(phase < R, 0, 1)

    def block_of(s):
        return (s // 2) * 2 * R + jnp.where(lax.rem(s, 2) == 0, my_r, 2 * R - 1 - my_r)

    weights = [(wq_h, wq), (wk_h, wk), (wv_h, wv), (wp_h, wp), (wop_h, wop), (woa_h, woa)]
    loads = [pltpu.make_async_copy(a, b, wsem.at[i]) for i, (a, b) in enumerate(weights)]
    for load in loads:
        load.start()

    barrier = pltpu.get_barrier_semaphore()

    @pl.loop(1, n * T)
    def _(o):
        other = lax.rem(me * T + t + o, n * T)
        pl.semaphore_signal(
            barrier, inc=1, device_id=(other // T, lax.rem(other, T)), device_id_type=MESH
        )

    pl.semaphore_wait(barrier, n * T - 1)

    def sibling(src, dst, ss, rs):
        return [
            pltpu.make_async_remote_copy(
                src_ref=src, dst_ref=dst, send_sem=ss.at[o - 1], recv_sem=rs.at[o - 1],
                device_id=(me, lax.rem(t + o, T)), device_id_type=MESH,
            )
            for o in range(1, T)
        ]

    tok_copies = sibling(tok, tokf.at[t], tok_ss, tok_rs)
    for c in tok_copies:
        c.start()
    tokf[t] = tok[...]
    for c in tok_copies:
        c.wait()

    Dt = tok.shape[1]
    square = jnp.zeros((L, 1), jnp.float32)
    for i in range(T):
        x = tokf[i].astype(jnp.float32)
        square += jnp.sum(x * x, axis=-1, keepdims=True)
    scale = lax.rsqrt(square / (T * Dt) + epsilon)
    for i in range(T):
        cols = slice(i * Dt, (i + 1) * Dt)
        x = tokf[i].astype(jnp.float32)
        nrm[:, cols] = (x * scale * ngain[:, cols]).astype(jnp.bfloat16)

    def head_norm(y, gain):
        y = y.reshape(Hh, HEAD_DIM, L)
        ms = jnp.mean(y * y, axis=1, keepdims=True)
        square_ids = [
            lax.broadcasted_iota(jnp.int32, (HEAD_DIM, HEAD_DIM), d) for d in (0, 1)
        ]
        column = jnp.sum(
            jnp.where(square_ids[0] == square_ids[1], gain[...], 0.0), axis=1, keepdims=True
        )
        return y * lax.rsqrt(ms + epsilon) * column[None]

    ghi, gmid, glow = split3(gT[...])
    row = lax.broadcasted_iota(jnp.int32, (PAD, L), 0)

    def gate_rows(h, sign, first):
        pad = jnp.where((row >= 3 - first) & (row < 6 - first), 1.0, 0.0)
        for k, part in enumerate((ghi, gmid, glow)):
            pad = jnp.where(row == k + first, sign * part[h : h + 1], pad)
        return pad.astype(jnp.bfloat16)

    loads[0].wait()
    q = head_norm(dot(wq[...], nrm[...], NT), qg) * HEAD_DIM ** (-0.5)
    qs[:, :HEAD_DIM] = q.astype(jnp.bfloat16)
    for h in range(Hh):
        qs[h, HEAD_DIM:KEY_ROWS] = gate_rows(h, 1.0, 3)

    def is_me(device):
        return (device[0] == me) & (device[1] == t)

    def q_home(h):
        return ((t * Hh + h) * C + out_r // T, lax.rem(out_r, T))

    def q_source(s):
        return (block_of(s), my_tp)

    def q_copy(h):
        return pltpu.make_async_remote_copy(
            src_ref=qs.at[h], dst_ref=qr.at[out_slot],
            send_sem=q_ss.at[h], recv_sem=q_rs.at[out_slot],
            device_id=q_home(h), device_id_type=MESH,
        )

    def q_arrival(s):
        return pltpu.make_async_remote_copy(
            src_ref=qs.at[0], dst_ref=qr.at[s],
            send_sem=q_ss.at[0], recv_sem=q_rs.at[s],
            device_id=q_source(s), device_id_type=MESH,
        )

    @pl.loop(0, Hh)
    def _(o):
        h = lax.rem(me + o, Hh)

        @pl.when(jnp.logical_not(is_me(q_home(h))))
        def _():
            q_copy(h).start()

        @pl.when(is_me(q_home(h)))
        def _():
            qr[out_slot] = qs[h]

    loads[1].wait()
    kvs[:, :HEAD_DIM] = head_norm(dot(wk[...], nrm[...], NT), kg).astype(jnp.bfloat16)
    for h in range(Hh):
        kvs[h, HEAD_DIM:KEY_ROWS] = gate_rows(h, -1.0, 0)
    loads[2].wait()
    kvs[:, KEY_ROWS:] = (
        dot(wv[...], nrm[...], NT).astype(jnp.bfloat16).reshape(Hh, HEAD_DIM, L)
    )

    def kv_home(k):
        return (t * span + k, relay)

    def kv_copy(k):
        return pltpu.make_async_remote_copy(
            src_ref=kvs.at[k // C], dst_ref=kvr.at[me],
            send_sem=kv_ss.at[k], recv_sem=kv_rs.at[me],
            device_id=kv_home(k), device_id_type=MESH,
        )

    def kv_arrival(j, tp):
        return pltpu.make_async_remote_copy(
            src_ref=kvs.at[0], dst_ref=kvr.at[j],
            send_sem=kv_ss.at[0], recv_sem=kv_rs.at[j],
            device_id=(me, tp), device_id_type=MESH,
        )

    def kv_forward(j, o):
        return pltpu.make_async_remote_copy(
            src_ref=kvr.at[j], dst_ref=kvr.at[j],
            send_sem=fw_ss.at[o - 1, j], recv_sem=kv_rs.at[j],
            device_id=(me, lax.rem(t + o, T)), device_id_type=MESH,
        )

    @pl.loop(0, span)
    def _(o):
        k = lax.rem(me + o, span)

        @pl.when(jnp.logical_not(is_me(kv_home(k))))
        def _():
            kv_copy(k).start()

        @pl.when(is_me(kv_home(k)))
        def _():
            kvr[me] = kvs[k // C]

    loads[3].wait()
    pool_input = dot(nrm[...], wp[...], NT).astype(jnp.bfloat16)
    ext[...] = pool_input[L - REACH :]
    rim_copy = pltpu.make_async_remote_copy(
        src_ref=ext, dst_ref=rim, send_sem=rim_ss, recv_sem=rim_rs,
        device_id=(lax.rem(me + 1, n), t), device_id_type=MESH,
    )

    rim_copy.start()
    rim_copy.wait()
    before = jnp.where(me == 0, 0.0, rim[...].astype(jnp.float32))
    current = pool_input.astype(jnp.float32)
    running = jnp.concatenate([before, current], axis=0)
    width_here = current.shape[1]
    channel = t * width_here + lax.broadcasted_iota(jnp.int32, (1, width_here), 1)
    group = channel // (POOL_WIDTH // POOL_GROUPS)
    counts = (me * L + 1 + lax.broadcasted_iota(jnp.int32, (L, 1), 0)).astype(jnp.float32)
    pooled = jnp.zeros_like(current)
    for g in range(POOL_GROUPS):
        lag = 2**g
        running = running + jnp.concatenate(
            [jnp.zeros((lag, width_here), jnp.float32), running[:-lag]], axis=0
        )
        average = running[REACH:] / jnp.minimum(counts, float(2 * lag))
        pooled = jnp.where(group == g, average, pooled)
    poolf[t] = (pooled - current).astype(jnp.bfloat16)
    pool_copies = sibling(poolf.at[t], poolf.at[t], pf_ss, pf_rs)
    for c in pool_copies:
        c.start()

    for c in pool_copies:
        c.wait()
    loads[4].wait()
    for i in range(T):
        part = dot(poolf[i], wop[i * width_here : (i + 1) * width_here], NN)
        if i == 0:
            total[...] = part
        else:
            total[...] += part

    top[...] = jnp.full(top.shape, masked_fill, jnp.float32)
    den[...] = jnp.zeros(den.shape, jnp.float32)
    acc[...] = jnp.zeros(acc.shape, jnp.float32)
    allowed = lax.broadcasted_iota(jnp.int32, (L, L), 0) <= lax.broadcasted_iota(
        jnp.int32, (L, L), 1
    )

    @pl.loop(0, Hh)
    def _(s):
        @pl.when(jnp.logical_not(is_me(q_source(s))))
        def _():
            q_arrival(s).wait_recv()

    def absorb(work, masked):
        logits = [dot(keys[m], qr[s], NN) for s, m, j in work]
        if masked:
            logits = [jnp.where(allowed, x, masked_fill) for x in logits]
        slots = [s for s, m, j in work]
        new = [jnp.maximum(top[s], jnp.max(x, axis=0, keepdims=True)) for s, x in zip(slots, logits)]
        w = [jnp.exp(x - m) for x, m in zip(logits, new)]
        parts = [
            dot(kvr[j, KEY_ROWS:], x.astype(jnp.bfloat16), NN) for (s, m, j), x in zip(work, w)
        ]
        for s, m, x, part in zip(slots, new, w, parts):
            old = jnp.exp(top[s] - m)
            top[s] = m
            den[s] = den[s] * old + jnp.sum(x, axis=0, keepdims=True)
            acc[s] = acc[s] * old + part

    def attend_halves(j):
        half = Hh // 2
        for m in range(2):
            keys[m] = jnp.transpose(kvr[j + m * span, :KEY_ROWS])
        p = lax.rem(j, 2 * R)
        low = 2 * (j // (2 * R)) + jnp.where(p > my_r, 1, 0) + jnp.where(p > 2 * R - 1 - my_r, 1, 0)
        diagonal = (p == my_r) | (p == 2 * R - 1 - my_r)
        absorb([(s, 0, j) for s in range(half, Hh)], False)

        @pl.when(diagonal)
        def _():
            absorb([(low, 0, j), (low + half, 1, j + span)], True)

        @pl.loop(low + jnp.where(diagonal, 1, 0), half)
        def _(s):
            absorb([(s, 0, j), (s + half, 1, j + span)], False)

    def attend(j):
        keys[0] = jnp.transpose(kvr[j, :KEY_ROWS])
        p = lax.rem(j, 2 * R)
        low = 2 * (j // (2 * R)) + jnp.where(p > my_r, 1, 0) + jnp.where(p > 2 * R - 1 - my_r, 1, 0)
        diagonal = (p == my_r) | (p == 2 * R - 1 - my_r)

        @pl.when(diagonal)
        def _():
            absorb([(low, 0, j)], True)

        low = low + jnp.where(diagonal, 1, 0)
        pairs = (Hh - low) // 2

        @pl.loop(0, pairs)
        def _(i):
            absorb([(low + 2 * i, 0, j), (low + 2 * i + 1, 0, j)], False)

        @pl.when(lax.rem(Hh - low, 2) == 1)
        def _():
            absorb([(Hh - 1, 0, j)], False)

    @pl.loop(0, span // T)
    def _(step):
        for u in range(T):
            k = step * T + lax.rem(seat - t - u + 2 * T, T)
            base = lax.rem(seat - k + span, span)
            for m in range(T):
                j = base + m * span

                @pl.when(jnp.logical_not((u == 0) & is_me((j, my_tp))))
                def _():
                    kv_arrival(j, lax.rem(t + 1, T)).wait_recv()

                if u == 0:
                    for o in range(1, T):
                        kv_forward(j, o).start()

            if T == 2 and span % (2 * R) == 0:
                attend_halves(base)
            else:

                @pl.loop(0, T)
                def _(m):
                    attend(base + m * span)

    def at_copy(s):
        return pltpu.make_async_remote_copy(
            src_ref=att_s.at[s], dst_ref=attf.at[my_tp, my_head],
            send_sem=at_ss.at[s], recv_sem=at_rs.at[my_head],
            device_id=q_source(s), device_id_type=MESH,
        )

    def at_arrival(h):
        return pltpu.make_async_remote_copy(
            src_ref=att_s.at[0], dst_ref=attf.at[t, h],
            send_sem=at_ss.at[0], recv_sem=at_rs.at[h],
            device_id=q_home(h), device_id_type=MESH,
        )

    @pl.loop(0, Hh)
    def _(s):
        att_s[s] = (acc[s] / den[s]).astype(jnp.bfloat16)

        @pl.when(jnp.logical_not(is_me(q_source(s))))
        def _():
            at_copy(s).start()

        @pl.when(is_me(q_source(s)))
        def _():
            attf[t, my_head] = att_s[s]

    @pl.loop(0, Hh)
    def _(h):
        @pl.when(jnp.logical_not(is_me(q_home(h))))
        def _():
            at_arrival(h).wait_recv()

    att_copies = sibling(attf.at[t], attf.at[t], af_ss, af_rs)
    for c in att_copies:
        c.start()
    loads[5].wait()

    def attn_part(i):
        rows = pl.ds(pl.multiple_of(i * F, F), F)
        return dot(attf[i].reshape(F, L), woa[rows], TN)

    result = total[...] + attn_part(t)
    for o in range(1, T):
        att_copies[o - 1].wait()
        result = result + attn_part(lax.rem(t - o + T, T))
    out[...] = result.astype(jnp.bfloat16)

    @pl.loop(0, span)
    def _(k):
        @pl.when(jnp.logical_not(is_me(kv_home(k))))
        def _():
            kv_copy(k).wait_send()

        for o in range(1, T):
            kv_forward(k * T + t, o).wait_send()

    @pl.loop(0, Hh)
    def _(h):
        @pl.when(jnp.logical_not(is_me(q_home(h))))
        def _():
            q_copy(h).wait_send()

        @pl.when(jnp.logical_not(is_me(q_source(h))))
        def _():
            at_copy(h).wait_send()


def solution(mesh):
    n, T = mesh.shape["sp"], mesh.shape["tp"]

    def per_device(
        tokens, norm_gain, query_weight, key_weight, value_weight, pool_weight,
        query_gain, key_gain, cum_gate, out_pool_weight, out_attn_weight,
    ):
        L, Dt = tokens.shape
        Hh = cum_gate.shape[1]
        R = n // Hh
        F = Hh * HEAD_DIM
        Fp = pool_weight.shape[0]
        bf, f32 = jnp.bfloat16, jnp.float32
        vmem = pl.BlockSpec(memory_space=pltpu.VMEM)
        hbm = pl.BlockSpec(memory_space=pl.ANY)
        dma = pltpu.SemaphoreType.DMA
        S = max(T - 1, 1)
        return pl.pallas_call(
            functools.partial(kernel, n, T, R, Hh),
            out_shape=jax.ShapeDtypeStruct((L, Dt), bf),
            in_specs=[vmem, vmem, hbm, hbm, hbm, hbm, vmem, vmem, vmem, hbm, hbm],
            out_specs=vmem,
            scratch_shapes=[
                pltpu.VMEM((T, L, Dt), bf),
                pltpu.VMEM((L, T * Dt), bf),
                pltpu.VMEM(query_weight.shape, bf),
                pltpu.VMEM(key_weight.shape, bf),
                pltpu.VMEM(value_weight.shape, bf),
                pltpu.VMEM(pool_weight.shape, bf),
                pltpu.VMEM(out_pool_weight.shape, bf),
                pltpu.VMEM(out_attn_weight.shape, bf),
                pltpu.VMEM((Hh, KEY_ROWS + HEAD_DIM, L), bf),
                pltpu.VMEM((Hh, KEY_ROWS, L), bf),
                pltpu.VMEM((n, KEY_ROWS + HEAD_DIM, L), bf),
                pltpu.VMEM((Hh, KEY_ROWS, L), bf),
                pltpu.VMEM((REACH, Fp), bf),
                pltpu.VMEM((REACH, Fp), bf),
                pltpu.VMEM((T, L, Fp), bf),
                pltpu.VMEM((Hh, HEAD_DIM, L), bf),
                pltpu.VMEM((T, Hh, HEAD_DIM, L), bf),
                pltpu.VMEM((L, Dt), f32),
                pltpu.VMEM((2, L, KEY_ROWS), bf),
                pltpu.VMEM((Hh, 1, L), f32),
                pltpu.VMEM((Hh, 1, L), f32),
                pltpu.VMEM((Hh, HEAD_DIM, L), f32),
                dma((6,)),
                dma((S,)), dma((S,)),
                dma((n // T,)), dma((n,)), dma((S, n)),
                dma((Hh,)), dma((Hh,)),
                dma, dma,
                dma((S,)), dma((S,)),
                dma((Hh,)), dma((Hh,)),
                dma((S,)), dma((S,)),
            ],
            compiler_params=pltpu.CompilerParams(
                collective_id=0, has_side_effects=True, vmem_limit_bytes=56 * 2**20
            ),
        )(
            tokens, norm_gain.reshape(1, -1), query_weight, key_weight, value_weight,
            pool_weight, query_gain.reshape(1, -1), key_gain.reshape(1, -1), cum_gate.T,
            out_pool_weight, out_attn_weight,
        )

    return jax.shard_map(
        per_device,
        mesh=mesh,
        in_specs=(
            P("sp", "tp"), P(), P("tp", None), P("tp", None), P("tp", None), P("tp", None),
            P(), P(), P("sp", "tp"), P(None, "tp"), P(None, "tp"),
        ),
        out_specs=P("sp", "tp"),
        check_vma=False,
    )
```

```python
import functools

import jax
import jax.numpy as jnp
from jax import lax
from jax.experimental import pallas as pl
from jax.experimental.pallas import tpu as pltpu
from jax.sharding import PartitionSpec as P

HEAD_DIM = 64
POOL_WIDTH = 1024
POOL_GROUPS = 4
PAD = 16
KEY_ROWS = HEAD_DIM + PAD
REACH = 2**POOL_GROUPS

epsilon = 1e-06
masked_fill = -1e30
MESH = pl.DeviceIdType.MESH
NT = (((1,), (1,)), ((), ()))
TN = (((0,), (0,)), ((), ()))
NN = (((1,), (0,)), ((), ()))


def dot(a, b, dims):
    return lax.dot_general(a, b, dims, preferred_element_type=jnp.float32)


def split3(x):
    hi = x.astype(jnp.bfloat16).astype(jnp.float32)
    mid = (x - hi).astype(jnp.bfloat16).astype(jnp.float32)
    low = (x - hi - mid).astype(jnp.bfloat16).astype(jnp.float32)
    return hi, mid, low


def kernel(
    n, T, R, Hh,
    tok, ngain, wq_h, wk_h, wv_h, wp_h, qg, kg, gT, wop_h, woa_h,
    out,
    tokf, nrm, wq, wk, wv, wp, wop, woa, kvs, qs, kvr, qr,
    ext, rim, poolf, att_s, attf, total, keys, top, den, acc,
    wsem, tok_ss, tok_rs, kv_ss, kv_rs, fw_ss, q_ss, q_rs, rim_ss, rim_rs,
    pf_ss, pf_rs, at_ss, at_rs, af_ss, af_rs,
):
    me = lax.axis_index("sp")
    t = lax.axis_index("tp")
    L = tok.shape[0]
    F = Hh * HEAD_DIM
    C = n // (T * Hh)
    span = n // T
    my_tp = me // (C * Hh)
    my_head = lax.rem(me // C, Hh)
    my_r = lax.rem(me, C) * T + t
    relay = lax.rem(me, T)
    seat = lax.rem(me, span)
    phase = lax.rem(me, 2 * R)
    out_r = jnp.where(phase < R, phase, 2 * R - 1 - phase)
    out_slot = 2 * (me // (2 * R)) + jnp.where(phase < R, 0, 1)

    def block_of(s):
        return (s // 2) * 2 * R + jnp.where(lax.rem(s, 2) == 0, my_r, 2 * R - 1 - my_r)

    weights = [(wq_h, wq), (wk_h, wk), (wv_h, wv), (wp_h, wp), (wop_h, wop), (woa_h, woa)]
    loads = [pltpu.make_async_copy(a, b, wsem.at[i]) for i, (a, b) in enumerate(weights)]
    for load in loads:
        load.start()

    barrier = pltpu.get_barrier_semaphore()

    @pl.loop(1, n * T)
    def _(o):
        other = lax.rem(me * T + t + o, n * T)
        pl.semaphore_signal(
            barrier, inc=1, device_id=(other // T, lax.rem(other, T)), device_id_type=MESH
        )

    pl.semaphore_wait(barrier, n * T - 1)

    def sibling(src, dst, ss, rs):
        return [
            pltpu.make_async_remote_copy(
                src_ref=src, dst_ref=dst, send_sem=ss.at[o - 1], recv_sem=rs.at[o - 1],
                device_id=(me, lax.rem(t + o, T)), device_id_type=MESH,
            )
            for o in range(1, T)
        ]

    tok_copies = sibling(tok, tokf.at[t], tok_ss, tok_rs)
    for c in tok_copies:
        c.start()
    tokf[t] = tok[...]
    Dt = tok.shape[1]
    x = tok[...].astype(jnp.float32)
    square = jnp.sum(x * x, axis=-1, keepdims=True)
    for o in range(1, T):
        tok_copies[o - 1].wait()
        x = tokf[lax.rem(t - o + T, T)].astype(jnp.float32)
        square += jnp.sum(x * x, axis=-1, keepdims=True)
    scale = lax.rsqrt(square / (T * Dt) + epsilon)
    for i in range(T):
        cols = slice(i * Dt, (i + 1) * Dt)
        x = tokf[i].astype(jnp.float32)
        nrm[:, cols] = (x * scale * ngain[:, cols]).astype(jnp.bfloat16)

    def head_norm(y, gain):
        y = y.reshape(Hh, HEAD_DIM, L)
        ms = jnp.mean(y * y, axis=1, keepdims=True)
        square_ids = [
            lax.broadcasted_iota(jnp.int32, (HEAD_DIM, HEAD_DIM), d) for d in (0, 1)
        ]
        column = jnp.sum(
            jnp.where(square_ids[0] == square_ids[1], gain[...], 0.0), axis=1, keepdims=True
        )
        return y * lax.rsqrt(ms + epsilon) * column[None]

    ghi, gmid, glow = split3(gT[...])
    row = lax.broadcasted_iota(jnp.int32, (PAD, L), 0)

    def gate_rows(h, sign, first):
        pad = jnp.where((row >= 3 - first) & (row < 6 - first), 1.0, 0.0)
        for k, part in enumerate((ghi, gmid, glow)):
            pad = jnp.where(row == k + first, sign * part[h : h + 1], pad)
        return pad.astype(jnp.bfloat16)

    loads[0].wait()
    q = head_norm(dot(wq[...], nrm[...], NT), qg) * HEAD_DIM ** (-0.5)
    qs[:, :HEAD_DIM] = q.astype(jnp.bfloat16)
    for h in range(Hh):
        qs[h, HEAD_DIM:KEY_ROWS] = gate_rows(h, 1.0, 3)

    def is_me(device):
        return (device[0] == me) & (device[1] == t)

    def q_home(h):
        return ((t * Hh + h) * C + out_r // T, lax.rem(out_r, T))

    def q_source(s):
        return (block_of(s), my_tp)

    def q_copy(h):
        return pltpu.make_async_remote_copy(
            src_ref=qs.at[h], dst_ref=qr.at[out_slot],
            send_sem=q_ss.at[h], recv_sem=q_rs.at[out_slot],
            device_id=q_home(h), device_id_type=MESH,
        )

    def q_arrival(s):
        return pltpu.make_async_remote_copy(
            src_ref=qs.at[0], dst_ref=qr.at[s],
            send_sem=q_ss.at[0], recv_sem=q_rs.at[s],
            device_id=q_source(s), device_id_type=MESH,
        )

    @pl.loop(0, Hh)
    def _(o):
        h = lax.rem(me + o, Hh)

        @pl.when(jnp.logical_not(is_me(q_home(h))))
        def _():
            q_copy(h).start()

        @pl.when(is_me(q_home(h)))
        def _():
            qr[out_slot] = qs[h]

    loads[1].wait()
    kvs[:, :HEAD_DIM] = head_norm(dot(wk[...], nrm[...], NT), kg).astype(jnp.bfloat16)
    for h in range(Hh):
        kvs[h, HEAD_DIM:KEY_ROWS] = gate_rows(h, -1.0, 0)
    loads[2].wait()
    kvs[:, KEY_ROWS:] = (
        dot(wv[...], nrm[...], NT).astype(jnp.bfloat16).reshape(Hh, HEAD_DIM, L)
    )

    def kv_home(k):
        return (t * span + k, relay)

    def kv_copy(k):
        return pltpu.make_async_remote_copy(
            src_ref=kvs.at[k // C], dst_ref=kvr.at[me],
            send_sem=kv_ss.at[k], recv_sem=kv_rs.at[me],
            device_id=kv_home(k), device_id_type=MESH,
        )

    def kv_arrival(j, tp):
        return pltpu.make_async_remote_copy(
            src_ref=kvs.at[0], dst_ref=kvr.at[j],
            send_sem=kv_ss.at[0], recv_sem=kv_rs.at[j],
            device_id=(me, tp), device_id_type=MESH,
        )

    def kv_forward(j, o):
        return pltpu.make_async_remote_copy(
            src_ref=kvr.at[j], dst_ref=kvr.at[j],
            send_sem=fw_ss.at[o - 1, j], recv_sem=kv_rs.at[j],
            device_id=(me, lax.rem(t + o, T)), device_id_type=MESH,
        )

    @pl.loop(0, span)
    def _(o):
        k = lax.rem(me + o, span)

        @pl.when(jnp.logical_not(is_me(kv_home(k))))
        def _():
            kv_copy(k).start()

        @pl.when(is_me(kv_home(k)))
        def _():
            kvr[me] = kvs[k // C]

    loads[3].wait()
    pool_input = dot(nrm[...], wp[...], NT).astype(jnp.bfloat16)
    ext[...] = pool_input[L - REACH :]
    rim_copy = pltpu.make_async_remote_copy(
        src_ref=ext, dst_ref=rim, send_sem=rim_ss, recv_sem=rim_rs,
        device_id=(lax.rem(me + 1, n), t), device_id_type=MESH,
    )

    rim_copy.start()
    rim_copy.wait()
    before = jnp.where(me == 0, 0.0, rim[...].astype(jnp.float32))
    current = pool_input.astype(jnp.float32)
    running = jnp.concatenate([before, current], axis=0)
    width_here = current.shape[1]
    channel = t * width_here + lax.broadcasted_iota(jnp.int32, (1, width_here), 1)
    group = channel // (POOL_WIDTH // POOL_GROUPS)
    counts = (me * L + 1 + lax.broadcasted_iota(jnp.int32, (L, 1), 0)).astype(jnp.float32)
    pooled = jnp.zeros_like(current)
    for g in range(POOL_GROUPS):
        lag = 2**g
        running = running + jnp.concatenate(
            [jnp.zeros((lag, width_here), jnp.float32), running[:-lag]], axis=0
        )
        average = running[REACH:] / jnp.minimum(counts, float(2 * lag))
        pooled = jnp.where(group == g, average, pooled)
    poolf[t] = (pooled - current).astype(jnp.bfloat16)
    pool_copies = sibling(poolf.at[t], poolf.at[t], pf_ss, pf_rs)
    for c in pool_copies:
        c.start()

    for c in pool_copies:
        c.wait()
    loads[4].wait()
    for i in range(T):
        part = dot(poolf[i], wop[i * width_here : (i + 1) * width_here], NN)
        if i == 0:
            total[...] = part
        else:
            total[...] += part

    top[...] = jnp.full(top.shape, masked_fill, jnp.float32)
    den[...] = jnp.zeros(den.shape, jnp.float32)
    acc[...] = jnp.zeros(acc.shape, jnp.float32)
    allowed = lax.broadcasted_iota(jnp.int32, (L, L), 0) <= lax.broadcasted_iota(
        jnp.int32, (L, L), 1
    )

    @pl.loop(0, Hh)
    def _(s):
        @pl.when(jnp.logical_not(is_me(q_source(s))))
        def _():
            q_arrival(s).wait_recv()

    def absorb(work, masked):
        logits = [dot(keys[m], qr[s], NN) for s, m, j in work]
        if masked:
            logits = [jnp.where(allowed, x, masked_fill) for x in logits]
        slots = [s for s, m, j in work]
        new = [jnp.maximum(top[s], jnp.max(x, axis=0, keepdims=True)) for s, x in zip(slots, logits)]
        w = [jnp.exp(x - m) for x, m in zip(logits, new)]
        parts = [
            dot(kvr[j, KEY_ROWS:], x.astype(jnp.bfloat16), NN) for (s, m, j), x in zip(work, w)
        ]
        for s, m, x, part in zip(slots, new, w, parts):
            old = jnp.exp(top[s] - m)
            top[s] = m
            den[s] = den[s] * old + jnp.sum(x, axis=0, keepdims=True)
            acc[s] = acc[s] * old + part

    def attend_halves(j):
        half = Hh // 2
        for m in range(2):
            keys[m] = jnp.transpose(kvr[j + m * span, :KEY_ROWS])
        p = lax.rem(j, 2 * R)
        low = 2 * (j // (2 * R)) + jnp.where(p > my_r, 1, 0) + jnp.where(p > 2 * R - 1 - my_r, 1, 0)
        diagonal = (p == my_r) | (p == 2 * R - 1 - my_r)
        absorb([(s, 0, j) for s in range(half, Hh)], False)

        @pl.when(diagonal)
        def _():
            absorb([(low, 0, j), (low + half, 1, j + span)], True)

        @pl.loop(low + jnp.where(diagonal, 1, 0), half)
        def _(s):
            absorb([(s, 0, j), (s + half, 1, j + span)], False)

    def attend(j):
        keys[0] = jnp.transpose(kvr[j, :KEY_ROWS])
        p = lax.rem(j, 2 * R)
        low = 2 * (j // (2 * R)) + jnp.where(p > my_r, 1, 0) + jnp.where(p > 2 * R - 1 - my_r, 1, 0)
        diagonal = (p == my_r) | (p == 2 * R - 1 - my_r)

        @pl.when(diagonal)
        def _():
            absorb([(low, 0, j)], True)

        low = low + jnp.where(diagonal, 1, 0)
        pairs = (Hh - low) // 2

        @pl.loop(0, pairs)
        def _(i):
            absorb([(low + 2 * i, 0, j), (low + 2 * i + 1, 0, j)], False)

        @pl.when(lax.rem(Hh - low, 2) == 1)
        def _():
            absorb([(Hh - 1, 0, j)], False)

    @pl.loop(0, span // T)
    def _(step):
        for u in range(T):
            k = step * T + lax.rem(seat - t - u + 2 * T, T)
            base = lax.rem(seat - k + span, span)
            for m in range(T):
                j = base + m * span

                @pl.when(jnp.logical_not((u == 0) & is_me((j, my_tp))))
                def _():
                    kv_arrival(j, lax.rem(t + 1, T)).wait_recv()

                if u == 0:
                    for o in range(1, T):
                        kv_forward(j, o).start()

            if T == 2 and span % (2 * R) == 0:
                attend_halves(base)
            else:

                @pl.loop(0, T)
                def _(m):
                    attend(base + m * span)

    def at_copy(s):
        return pltpu.make_async_remote_copy(
            src_ref=att_s.at[s], dst_ref=attf.at[my_tp, my_head],
            send_sem=at_ss.at[s], recv_sem=at_rs.at[my_head],
            device_id=q_source(s), device_id_type=MESH,
        )

    def at_arrival(h):
        return pltpu.make_async_remote_copy(
            src_ref=att_s.at[0], dst_ref=attf.at[t, h],
            send_sem=at_ss.at[0], recv_sem=at_rs.at[h],
            device_id=q_home(h), device_id_type=MESH,
        )

    @pl.loop(0, Hh)
    def _(s):
        att_s[s] = (acc[s] / den[s]).astype(jnp.bfloat16)

        @pl.when(jnp.logical_not(is_me(q_source(s))))
        def _():
            at_copy(s).start()

        @pl.when(is_me(q_source(s)))
        def _():
            attf[t, my_head] = att_s[s]

    @pl.loop(0, Hh)
    def _(h):
        @pl.when(jnp.logical_not(is_me(q_home(h))))
        def _():
            at_arrival(h).wait_recv()

    att_copies = sibling(attf.at[t], attf.at[t], af_ss, af_rs)
    for c in att_copies:
        c.start()
    loads[5].wait()

    def attn_part(i):
        rows = pl.ds(pl.multiple_of(i * F, F), F)
        return dot(attf[i].reshape(F, L), woa[rows], TN)

    result = total[...] + attn_part(t)
    for o in range(1, T):
        att_copies[o - 1].wait()
        result = result + attn_part(lax.rem(t - o + T, T))
    out[...] = result.astype(jnp.bfloat16)

    @pl.loop(0, span)
    def _(k):
        @pl.when(jnp.logical_not(is_me(kv_home(k))))
        def _():
            kv_copy(k).wait_send()

        for o in range(1, T):
            kv_forward(k * T + t, o).wait_send()

    @pl.loop(0, Hh)
    def _(h):
        @pl.when(jnp.logical_not(is_me(q_home(h))))
        def _():
            q_copy(h).wait_send()

        @pl.when(jnp.logical_not(is_me(q_source(h))))
        def _():
            at_copy(h).wait_send()


def solution(mesh):
    n, T = mesh.shape["sp"], mesh.shape["tp"]

    def per_device(
        tokens, norm_gain, query_weight, key_weight, value_weight, pool_weight,
        query_gain, key_gain, cum_gate, out_pool_weight, out_attn_weight,
    ):
        L, Dt = tokens.shape
        Hh = cum_gate.shape[1]
        R = n // Hh
        F = Hh * HEAD_DIM
        Fp = pool_weight.shape[0]
        bf, f32 = jnp.bfloat16, jnp.float32
        vmem = pl.BlockSpec(memory_space=pltpu.VMEM)
        hbm = pl.BlockSpec(memory_space=pl.ANY)
        dma = pltpu.SemaphoreType.DMA
        S = max(T - 1, 1)
        return pl.pallas_call(
            functools.partial(kernel, n, T, R, Hh),
            out_shape=jax.ShapeDtypeStruct((L, Dt), bf),
            in_specs=[vmem, vmem, hbm, hbm, hbm, hbm, vmem, vmem, vmem, hbm, hbm],
            out_specs=vmem,
            scratch_shapes=[
                pltpu.VMEM((T, L, Dt), bf),
                pltpu.VMEM((L, T * Dt), bf),
                pltpu.VMEM(query_weight.shape, bf),
                pltpu.VMEM(key_weight.shape, bf),
                pltpu.VMEM(value_weight.shape, bf),
                pltpu.VMEM(pool_weight.shape, bf),
                pltpu.VMEM(out_pool_weight.shape, bf),
                pltpu.VMEM(out_attn_weight.shape, bf),
                pltpu.VMEM((Hh, KEY_ROWS + HEAD_DIM, L), bf),
                pltpu.VMEM((Hh, KEY_ROWS, L), bf),
                pltpu.VMEM((n, KEY_ROWS + HEAD_DIM, L), bf),
                pltpu.VMEM((Hh, KEY_ROWS, L), bf),
                pltpu.VMEM((REACH, Fp), bf),
                pltpu.VMEM((REACH, Fp), bf),
                pltpu.VMEM((T, L, Fp), bf),
                pltpu.VMEM((Hh, HEAD_DIM, L), bf),
                pltpu.VMEM((T, Hh, HEAD_DIM, L), bf),
                pltpu.VMEM((L, Dt), f32),
                pltpu.VMEM((2, L, KEY_ROWS), bf),
                pltpu.VMEM((Hh, 1, L), f32),
                pltpu.VMEM((Hh, 1, L), f32),
                pltpu.VMEM((Hh, HEAD_DIM, L), f32),
                dma((6,)),
                dma((S,)), dma((S,)),
                dma((n // T,)), dma((n,)), dma((S, n)),
                dma((Hh,)), dma((Hh,)),
                dma, dma,
                dma((S,)), dma((S,)),
                dma((Hh,)), dma((Hh,)),
                dma((S,)), dma((S,)),
            ],
            compiler_params=pltpu.CompilerParams(
                collective_id=0, has_side_effects=True, vmem_limit_bytes=56 * 2**20
            ),
        )(
            tokens, norm_gain.reshape(1, -1), query_weight, key_weight, value_weight,
            pool_weight, query_gain.reshape(1, -1), key_gain.reshape(1, -1), cum_gate.T,
            out_pool_weight, out_attn_weight,
        )

    return jax.shard_map(
        per_device,
        mesh=mesh,
        in_specs=(
            P("sp", "tp"), P(), P("tp", None), P("tp", None), P("tp", None), P("tp", None),
            P(), P(), P("sp", "tp"), P(None, "tp"), P(None, "tp"),
        ),
        out_specs=P("sp", "tp"),
        check_vma=False,
    )
```
